32 devices in a mesh: ep: 8 (over z, core), tp: 4 (over y, x).
Axes of the slice: x: 2, y: 2, z: 4, core: 2. Of those that a mesh axis runs over, the one named last changes fastest.
Arguments:
- recurrence_queries: bfloat16 [4096, 2048], P('ep', 'tp'), may hold values from -6 to 6
- forget_preact: bfloat16 [4096, 2048], P('ep', 'tp')
- recurrence_values: bfloat16 [4096, 2048], P('ep', 'tp'), may hold values from -6 to 6
- output_gate_preact: bfloat16 [4096, 2048], P('ep', 'tp'), may hold values from -6 to 6
- forget_floor_logits: float32 [2048], P('tp')
- surge_log_decay: float32 [4096, 16], P('ep', 'tp'), may hold values from -0.7 to 0
- head_norm_gain: float32 [128], replicated, may hold values from 0.1 to 1.9
- recurrence_out_weight: bfloat16 [2048, 2048], P(None, 'tp'), may hold values from -0.125 to 0.125
- second_micro_rows: bfloat16 [1024, 2048], P('ep'), may hold values from -6 to 6
- expert_norm_gain: float32 [2048], replicated, may hold values from 0.1 to 1.9
- row_group_index: int32 [1024], P('ep'), may hold values from 0 to 3, as said below
- group_expert_index: int32 [1024, 2], P('ep'), may hold values from 0 to 7, as said below
- chosen_expert_weight: float32 [1024, 2], P('ep'), may hold values from 0.2 to 1
- expert_gate_weight: bfloat16 [32, 2048, 4096], P('ep', None, 'tp'), may hold values from -0.125 to 0.125
- expert_up_weight: bfloat16 [32, 2048, 4096], P('ep', None, 'tp'), may hold values from -0.125 to 0.125
- expert_down_weight: bfloat16 [32, 4096, 2048], P('ep', None, 'tp'), may hold values from -0.09375 to 0.09375
Outputs:
- mixed: bfloat16 [4096, 2048], P('ep', 'tp')
- expert_out: bfloat16 [1024, 2048], P('ep', 'tp')
The draws below stay inside these ranges and needn't reach their ends.
Inputs may be any that keep to these rules, and one draw needn't show every extreme that they name: group_expert_index names two different experts of the row's group; the expert's number is row_group_index * 8 + group_expert_index. Among the rows of one index of ep no expert is named more than 12 times, and some expert exactly 12 times. `group_expert_index`: the two entries of a row differ.
All inputs are finite; a program needn't handle non-finite values.
Results may differ from the reference program's by a relative error of at most 0.009.
Values may be sent and summed in bfloat16 or wider, within the bound.
No kernel may reach another device: no remote copies, remote signals or barrier semaphores. Data moves between devices by JAX's collectives and lax.ppermute only.
A program may use at most 128 MiB of HBM per device.

```python
import math
import jax
import jax.numpy as jnp
from jax import lax

D = 2048
HEADS = 16
KEY_DIM = 128
VAL_DIM = 128
BLOCK = 64
EXPERTS = 32
GROUPS = 4
FF = 4096
TOK_M = 512
LENGTH = 4096
EXP_ROWS = 128
ALL_ROWS = 1024
CAP = 12
N_EP = 8


def draw_forget_preact(key, part):
    array_shape = (LENGTH, HEADS * KEY_DIM)
    base = jax.random.normal(jax.random.fold_in(key, 1), array_shape, jnp.float32)
    shift = jax.random.uniform(jax.random.fold_in(key, 2), (LENGTH // TOK_M, 1), jnp.float32, -1.5, 1.5)
    return (base + jnp.repeat(shift, TOK_M, axis=0)).astype(jnp.bfloat16)


def draw_forget_floor_logits(key, part):
    share = 0.5
    slow = jax.random.uniform(jax.random.fold_in(key, 21), (HEADS, 1), jnp.float32) < share
    spread = jax.random.uniform(jax.random.fold_in(key, 22), (HEADS, KEY_DIM), jnp.float32, 0.5, 2.0) / LENGTH
    quick = jnp.exp(jax.random.uniform(jax.random.fold_in(key, 23), (HEADS, KEY_DIM), jnp.float32, math.log(0.02), math.log(0.066)))
    rate = jnp.where(slow, spread, quick)
    return jnp.log((1.0 - rate) / rate).reshape(-1).astype(jnp.float32)


def draw_surge_log_decay(key, part):
    hit = jax.random.uniform(jax.random.fold_in(key, 31), (LENGTH, HEADS), jnp.float32) < 6.0 / LENGTH
    depth = jnp.log(jax.random.uniform(jax.random.fold_in(key, 32), (LENGTH, HEADS), jnp.float32, 0.5, 0.8))
    return jnp.where(hit, depth, 0.0).astype(jnp.float32)


def route_parts(key):
    block_total = ALL_ROWS // EXP_ROWS
    unit_rows = EXP_ROWS // 32
    patterns = jnp.array([[12, 8, 6, 6], [12, 10, 6, 4]], jnp.int32) * unit_rows
    chosen = jax.random.randint(jax.random.fold_in(key, 11), (block_total,), 0, 2)

    def one_block(index):
        sub_key = jax.random.fold_in(key, 100 + index)
        counts = patterns[chosen[index]]
        counts = counts[jax.random.permutation(jax.random.fold_in(sub_key, 1), 4)]
        bounds = jnp.cumsum(counts)
        position = jnp.arange(EXP_ROWS, dtype=jnp.int32)
        group = jnp.sum((position[:, None] >= bounds[None, :]).astype(jnp.int32), axis=1)
        begins = bounds - counts
        within = position - begins[group]
        orders = jnp.stack([jax.random.permutation(jax.random.fold_in(sub_key, 2 + g), 8) for g in range(4)])
        first = orders[group, within % 8]
        second = orders[group, (within + 4) % 8]
        row_perm = jax.random.permutation(jax.random.fold_in(sub_key, 9), EXP_ROWS)
        inverse = jnp.argsort(row_perm)
        return (group[inverse], jnp.stack([first, second], axis=1)[inverse])
    groups, local_sets = jax.vmap(one_block)(jnp.arange(block_total))
    return (groups.reshape(-1).astype(jnp.int32), local_sets.reshape(-1, 2).astype(jnp.int32))


def draw_row_group_index(key, part):
    return route_parts(jax.random.fold_in(key, 7))[0]


def draw_group_expert_index(key, part):
    return route_parts(jax.random.fold_in(key, 7))[1]


def block_scale(own_key, dims, split, low, largest):
    factor_of, own = 1.0, jax.random.fold_in(own_key, 6)
    for axis_at, shards_of in split:
        draws = jnp.exp(jax.random.uniform(jax.random.fold_in(own, axis_at), (shards_of,), jnp.float32, low / len(split), largest / len(split)))
        factor_of = factor_of * jnp.repeat(draws, dims[axis_at] // shards_of).reshape([-1 if axis == axis_at else 1 for axis in range(len(dims))])
    return factor_of


def bell_draw(key, dims, scale, reach, shards=(), kind=jnp.bfloat16):
    result = scale * jax.random.normal(key, dims, jnp.float32)
    if shards:
        result = result * block_scale(key, dims, shards, -0.22, 0.18)
    return jnp.clip(result, -reach, reach).astype(kind)


def setup_inputs(seed: int = 0) -> dict:
    splits = jax.random.split(jax.random.key(seed), 17)
    return {
        "recurrence_queries": bell_draw(splits[0], (LENGTH, HEADS * KEY_DIM), 1.0, 6.0, ((0, 8), (1, 4))),
        "forget_preact": draw_forget_preact(jax.random.fold_in(splits[16], 71), 0),
        "recurrence_values": bell_draw(splits[2], (LENGTH, HEADS * VAL_DIM), 1.0, 6.0, ((0, 8), (1, 4))),
        "output_gate_preact": bell_draw(splits[3], (LENGTH, HEADS * VAL_DIM), 1.0, 6.0, ((0, 8), (1, 4))),
        "forget_floor_logits": draw_forget_floor_logits(jax.random.fold_in(splits[16], 71), 0),
        "surge_log_decay": draw_surge_log_decay(jax.random.fold_in(splits[16], 71), 0),
        "head_norm_gain": jnp.clip(1.0 + 0.18 * jax.random.normal(splits[6], (VAL_DIM,), jnp.float32), 0.1, 1.9),
        "recurrence_out_weight": bell_draw(splits[7], (HEADS * VAL_DIM, D), (HEADS * VAL_DIM) ** -0.5, 0.125, ((1, 4),)),
        "second_micro_rows": bell_draw(splits[8], (ALL_ROWS, D), 1.0, 6.0, ((0, 8),)),
        "expert_norm_gain": jnp.clip(1.0 + 0.18 * jax.random.normal(splits[9], (D,), jnp.float32), 0.1, 1.9),
        "row_group_index": draw_row_group_index(jax.random.fold_in(splits[16], 71), 0),
        "group_expert_index": draw_group_expert_index(jax.random.fold_in(splits[16], 71), 0),
        "chosen_expert_weight": jnp.clip(0.2 + 0.8 * jax.random.uniform(splits[12], (ALL_ROWS, 2), jnp.float32) ** block_scale(splits[12], (ALL_ROWS, 2), ((0, 8),), -0.2, 0.2), 0.2, 1.0),
        "expert_gate_weight": bell_draw(splits[13], (EXPERTS, D, FF), D ** -0.5, 0.125, ((0, 8), (2, 4))),
        "expert_up_weight": bell_draw(splits[14], (EXPERTS, D, FF), D ** -0.5, 0.125, ((0, 8), (2, 4))),
        "expert_down_weight": bell_draw(splits[15], (EXPERTS, FF, D), FF ** -0.5, 0.09375, ((0, 8), (2, 4))),
    }


NORM_EPS = 1e-06
EXACT_PRECISION = lax.Precision.HIGHEST

def block_recurrence(query_activated, key_in, value_act, forget_log_value, state_init):
    block_len = query_activated.shape[1]
    causal = (jnp.arange(block_len)[:, None] >= jnp.arange(block_len)[None, :])[:, :, None, None]

    def block_step(current_state, block_inputs):
        query_tile, key_tile, value_tile, g_block = block_inputs
        running_total_sum = jnp.cumsum(g_block, axis=0)
        state_carried_out = jnp.einsum('cra,ran->crn', query_tile * jnp.exp(running_total_sum), current_state, precision=EXACT_PRECISION)
        relative = jnp.where(causal, running_total_sum[:, None] - running_total_sum[None, :], 0.0)
        decays = jnp.where(causal, jnp.exp(relative), 0.0)
        scores = jnp.einsum('thk,tshk,shk->hts', query_tile, decays, key_tile, precision=EXACT_PRECISION)
        output = state_carried_out + jnp.einsum('hts,shv->thv', scores, value_tile, precision=EXACT_PRECISION)
        final_log_value = running_total_sum[-1]
        current_state = jnp.exp(final_log_value)[:, :, None] * current_state + jnp.einsum('ceu,cex->eux', key_tile * jnp.exp(final_log_value[None] - running_total_sum), value_tile, precision=EXACT_PRECISION)
        return (current_state, output)
    return lax.scan(block_step, state_init, (query_activated, key_in, value_act, forget_log_value))

def token_mixing_layer(recurrence_queries, forget_preact, recurrence_values, output_gate_preact, forget_floor_logits, surge_log_decay, head_norm_gain, recurrence_out_weight):
    sequence_length = recurrence_queries.shape[0]
    number_of_heads = surge_log_decay.shape[1]
    key_feature_width = recurrence_queries.shape[1] // number_of_heads
    val_dim = recurrence_values.shape[1] // number_of_heads
    rate = jax.nn.sigmoid(-forget_floor_logits)
    input_gate_value = rate * jax.nn.sigmoid(-forget_preact.astype(jnp.float32))
    forget_log_value = jnp.log1p(-input_gate_value).reshape(sequence_length, number_of_heads, key_feature_width) + surge_log_decay[:, :, None]
    query_activated = jax.nn.silu(recurrence_queries.astype(jnp.float32)).reshape(sequence_length, number_of_heads, key_feature_width)
    key_in = input_gate_value.reshape(sequence_length, number_of_heads, key_feature_width)
    value_act = recurrence_values.astype(jnp.float32).reshape(sequence_length, number_of_heads, val_dim)
    block_count = sequence_length // BLOCK

    def to_blocks(array):
        return array.reshape(block_count, BLOCK, number_of_heads, array.shape[-1])
    state_init = jnp.zeros((number_of_heads, key_feature_width, val_dim), jnp.float32)
    _, recur_out = block_recurrence(to_blocks(query_activated), to_blocks(key_in), to_blocks(value_act), to_blocks(forget_log_value), state_init)
    recur_out = recur_out.reshape(sequence_length, number_of_heads, val_dim)
    normed = recur_out * lax.rsqrt(lax.optimization_barrier(jnp.mean(recur_out * recur_out, axis=-1, keepdims=True)) + NORM_EPS) * head_norm_gain
    gate_act = jax.nn.silu(output_gate_preact.astype(jnp.float32)).reshape(sequence_length, number_of_heads, val_dim)
    gated_heads = (normed * gate_act).reshape(sequence_length, number_of_heads * val_dim).astype(jnp.bfloat16)
    return jnp.dot(gated_heads, recurrence_out_weight, preferred_element_type=jnp.float32).astype(jnp.bfloat16)

def routed_experts(second_micro_rows, expert_norm_gain, row_group_index, group_expert_index, chosen_expert_weight, expert_gate_weight, expert_up_weight, expert_down_weight):
    row_count = second_micro_rows.shape[0]
    model_width = second_micro_rows.shape[1]
    expert_count = expert_gate_weight.shape[0]
    per_group = expert_count // GROUPS
    rows_float = second_micro_rows.astype(jnp.float32)
    normed_rows = (rows_float * lax.rsqrt(lax.optimization_barrier(jnp.mean(rows_float * rows_float, axis=-1, keepdims=True)) + NORM_EPS) * expert_norm_gain).astype(jnp.bfloat16)
    expert_choice = (row_group_index[:, None] * per_group + group_expert_index).astype(jnp.int32)
    flat_expert = expert_choice.reshape(-1)
    onehot = (flat_expert[:, None] == jnp.arange(expert_count, dtype=jnp.int32)[None, :]).astype(jnp.int32)
    rank_index = lax.optimization_barrier(jnp.sum((jnp.cumsum(onehot, axis=0) - onehot) * onehot, axis=1)).astype(jnp.int32)
    room_size = N_EP * CAP
    slot_index = (flat_expert * room_size + rank_index).astype(jnp.int32)
    owner_row = jnp.full((expert_count * room_size,), row_count, jnp.int32).at[slot_index].set((jnp.arange(2 * row_count) // 2).astype(jnp.int32))
    padded = jnp.concatenate([normed_rows, jnp.zeros((1, model_width), jnp.bfloat16)], axis=0)

    def expert_block(operands):
        row_index, gate_mat, up_mat, down_mat = operands
        gathered_rows = padded[row_index]
        gate_act = jnp.dot(gathered_rows, gate_mat, preferred_element_type=jnp.float32)
        up_act = jnp.dot(gathered_rows, up_mat, preferred_element_type=jnp.float32)
        expert_hidden = (jax.nn.silu(gate_act) * up_act).astype(jnp.bfloat16)
        return jnp.dot(expert_hidden, down_mat, preferred_element_type=jnp.float32).astype(jnp.bfloat16)
    expert_result = lax.map(expert_block, (owner_row.reshape(expert_count, room_size), expert_gate_weight, expert_up_weight, expert_down_weight))
    picked = expert_result.reshape(expert_count * room_size, model_width)[slot_index]
    picked = picked.reshape(row_count, 2, model_width).astype(jnp.float32)
    return lax.optimization_barrier(jnp.sum(picked * chosen_expert_weight[:, :, None], axis=1)).astype(jnp.bfloat16)

def reference(recurrence_queries, forget_preact, recurrence_values, output_gate_preact, forget_floor_logits, surge_log_decay, head_norm_gain, recurrence_out_weight, second_micro_rows, expert_norm_gain, row_group_index, group_expert_index, chosen_expert_weight, expert_gate_weight, expert_up_weight, expert_down_weight):
    mixed = token_mixing_layer(recurrence_queries, forget_preact, recurrence_values, output_gate_preact, forget_floor_logits, surge_log_decay, head_norm_gain, recurrence_out_weight)
    expert_out = routed_experts(second_micro_rows, expert_norm_gain, row_group_index, group_expert_index, chosen_expert_weight, expert_gate_weight, expert_up_weight, expert_down_weight)
    return (mixed, expert_out)
```

```python
import jax
import jax.numpy as jnp
import numpy as np
from jax import lax
from jax.experimental import pallas as pl
from jax.experimental.pallas import tpu as pltpu
from jax.sharding import PartitionSpec as P


BLOCK = 64
CHUNK = 128
GROUPS = 4
CAP = 12
TAIL = 16
NORM_EPS = 1e-06
F32, BF16 = jnp.float32, jnp.bfloat16
EXACT_PRECISION = lax.Precision.HIGHEST


def entering(value, axis, join, neutral):
    count, mine = (lax.axis_size(axis), lax.axis_index(axis))
    pieces = jax.tree.map(lambda part: lax.all_gather(part, axis), value)
    total = jax.tree.map(
        lambda part, zero: jnp.full_like(part, 0) + jnp.asarray(zero, part.dtype), value, neutral
    )

    def hop(position, total):
        longer = join(total, jax.tree.map(lambda part: part[position], pieces))
        return jax.tree.map(lambda new, old: jnp.where(position < mine, new, old), longer, total)

    return lax.fori_loop(0, count - 1, hop, total)


def block_recurrence(query_activated, key_in, value_act, forget_log_value, state_init):
    block_len = query_activated.shape[1]
    causal = (jnp.arange(block_len)[:, None] >= jnp.arange(block_len)[None, :])[:, :, None, None]

    def block_step(current_state, block_inputs):
        query_tile, key_tile, value_tile, g_block = block_inputs
        running_total_sum = jnp.cumsum(g_block, axis=0)
        state_carried_out = jnp.einsum(
            "cra,ran->crn",
            query_tile * jnp.exp(running_total_sum),
            current_state,
            precision=EXACT_PRECISION,
        )
        relative = jnp.where(causal, running_total_sum[:, None] - running_total_sum[None, :], 0.0)
        decays = jnp.where(causal, jnp.exp(relative), 0.0)
        scores = jnp.einsum(
            "thk,tshk,shk->hts", query_tile, decays, key_tile, precision=EXACT_PRECISION
        )
        output = state_carried_out + jnp.einsum(
            "hts,shv->thv", scores, value_tile, precision=EXACT_PRECISION
        )
        final_log_value = running_total_sum[-1]
        current_state = jnp.exp(final_log_value)[:, :, None] * current_state + jnp.einsum(
            "ceu,cex->eux",
            key_tile * jnp.exp(final_log_value[None] - running_total_sum),
            value_tile,
            precision=EXACT_PRECISION,
        )
        return (current_state, output)

    return lax.scan(block_step, state_init, (query_activated, key_in, value_act, forget_log_value))


def carry_join(earlier, later):
    return (earlier[0] * later[0], later[0][:, :, None] * earlier[1] + later[1])


def token_mixing_layer(
    recurrence_queries,
    forget_preact,
    recurrence_values,
    output_gate_preact,
    forget_floor_logits,
    surge_log_decay,
    head_norm_gain,
    recurrence_out_weight,
):
    token_inputs = recurrence_queries.shape[0]
    number_of_heads = surge_log_decay.shape[1]
    key_feature_width = recurrence_queries.shape[1] // number_of_heads
    val_dim = recurrence_values.shape[1] // number_of_heads
    rate = jax.nn.sigmoid(-forget_floor_logits)
    input_gate_value = rate * jax.nn.sigmoid(-forget_preact.astype(jnp.float32))
    forget_log_value = (
        jnp.log1p(-input_gate_value).reshape(token_inputs, number_of_heads, key_feature_width)
        + surge_log_decay[:, :, None]
    )
    query_activated = jax.nn.silu(recurrence_queries.astype(jnp.float32)).reshape(
        token_inputs, number_of_heads, key_feature_width
    )
    key_in = input_gate_value.reshape(token_inputs, number_of_heads, key_feature_width)
    value_act = recurrence_values.astype(jnp.float32).reshape(
        token_inputs, number_of_heads, val_dim
    )
    block_count = token_inputs // BLOCK

    def to_blocks(array):
        return array.reshape(block_count, BLOCK, number_of_heads, array.shape[-1])

    state_init = jnp.zeros((number_of_heads, key_feature_width, val_dim), jnp.float32)
    ending, recur_out = block_recurrence(
        to_blocks(query_activated),
        to_blocks(key_in),
        to_blocks(value_act),
        to_blocks(forget_log_value),
        state_init,
    )
    recur_out = recur_out.reshape(token_inputs, number_of_heads, val_dim)
    total_decay = jnp.exp(jnp.sum(forget_log_value, axis=0))
    incoming_state = entering(
        (total_decay, ending),
        "ep",
        carry_join,
        (jnp.ones_like(total_decay), jnp.zeros_like(ending)),
    )[1]
    running_state = jnp.cumsum(forget_log_value, axis=0)
    recur_out = recur_out + jnp.einsum(
        "cra,ran->crn",
        query_activated * jnp.exp(running_state),
        incoming_state,
        precision=EXACT_PRECISION,
    )
    normed = (
        recur_out
        * lax.rsqrt(jnp.mean(recur_out * recur_out, axis=-1, keepdims=True) + NORM_EPS)
        * head_norm_gain
    )
    gate_act = jax.nn.silu(output_gate_preact.astype(jnp.float32)).reshape(
        token_inputs, number_of_heads, val_dim
    )
    gated_heads = (
        (normed * gate_act).reshape(token_inputs, number_of_heads * val_dim).astype(jnp.bfloat16)
    )
    return jnp.dot(
        lax.all_gather(gated_heads, "tp", axis=1, tiled=True),
        recurrence_out_weight,
        preferred_element_type=jnp.float32,
    ).astype(jnp.bfloat16)


def routed_experts(
    second_micro_rows,
    expert_norm_gain,
    row_group_index,
    group_expert_index,
    chosen_expert_weight,
    expert_gate_weight,
    expert_up_weight,
    expert_down_weight,
):
    row_count = second_micro_rows.shape[0]
    model_width = second_micro_rows.shape[1]
    columns = model_width // lax.axis_size("tp")
    local_count = expert_gate_weight.shape[0]
    expert_count = local_count * lax.axis_size("ep")
    per_group = expert_count // GROUPS
    rows_float = second_micro_rows.astype(jnp.float32)
    normed_rows = (
        rows_float
        * lax.rsqrt(jnp.mean(rows_float * rows_float, axis=-1, keepdims=True) + NORM_EPS)
        * expert_norm_gain
    ).astype(jnp.bfloat16)
    flat_expert = (row_group_index[:, None] * per_group + group_expert_index).reshape(-1)
    onehot = (flat_expert[:, None] == jnp.arange(expert_count, dtype=jnp.int32)[None, :]).astype(
        jnp.int32
    )
    rank_index = jnp.sum((jnp.cumsum(onehot, axis=0) - onehot) * onehot, axis=1)
    slot_index = flat_expert * CAP + rank_index
    owner_row = (
        jnp.full((expert_count * CAP,), row_count, jnp.int32)
        .at[slot_index]
        .set(jnp.arange(2 * row_count) // 2)
    )
    col_part = lax.dynamic_slice_in_dim(normed_rows, lax.axis_index("tp") * columns, columns, 1)
    padded = jnp.concatenate([col_part, jnp.zeros((1, columns), jnp.bfloat16)], axis=0)
    outgoing = padded[owner_row].reshape(expert_count, CAP, columns)
    arrived = lax.all_to_all(outgoing, "ep", split_axis=0, concat_axis=1, tiled=True)
    arrived = lax.all_gather(arrived, "tp", axis=2, tiled=True)
    gate_act = jnp.einsum(
        "erd,edf->erf", arrived, expert_gate_weight, preferred_element_type=jnp.float32
    )
    up_act = jnp.einsum(
        "erd,edf->erf", arrived, expert_up_weight, preferred_element_type=jnp.float32
    )
    hidden = (jax.nn.silu(gate_act) * up_act).astype(jnp.bfloat16)
    result = jnp.einsum(
        "erf,efd->erd",
        lax.all_gather(hidden, "tp", axis=2, tiled=True),
        expert_down_weight,
        preferred_element_type=jnp.float32,
    ).astype(jnp.bfloat16)
    returned = lax.all_to_all(result, "ep", split_axis=1, concat_axis=0, tiled=True)
    picked = returned.reshape(expert_count * CAP, expert_down_weight.shape[2])[slot_index]
    picked = picked.reshape(row_count, 2, expert_down_weight.shape[2]).astype(jnp.float32)
    return jnp.sum(picked * chosen_expert_weight[:, :, None], axis=1).astype(jnp.bfloat16)


def plain(
    recurrence_queries,
    forget_preact,
    recurrence_values,
    output_gate_preact,
    forget_floor_logits,
    surge_log_decay,
    head_norm_gain,
    recurrence_out_weight,
    second_micro_rows,
    expert_norm_gain,
    row_group_index,
    group_expert_index,
    chosen_expert_weight,
    expert_gate_weight,
    expert_up_weight,
    expert_down_weight,
):
    mixed = token_mixing_layer(
        recurrence_queries,
        forget_preact,
        recurrence_values,
        output_gate_preact,
        forget_floor_logits,
        surge_log_decay,
        head_norm_gain,
        recurrence_out_weight,
    )
    expert_out = routed_experts(
        second_micro_rows,
        expert_norm_gain,
        row_group_index,
        group_expert_index,
        chosen_expert_weight,
        expert_gate_weight,
        expert_up_weight,
        expert_down_weight,
    )
    return (mixed, expert_out)


def dot_nn(a, b):
    return lax.dot_general(a, b, (((1,), (0,)), ((), ())), preferred_element_type=F32)


def dot_nt(a, b):
    return lax.dot_general(a, b, (((1,), (1,)), ((), ())), preferred_element_type=F32)


def dot_tn(a, b):
    return lax.dot_general(a, b, (((0,), (0,)), ((), ())), preferred_element_type=F32)


def sigmoid(x):
    return 1.0 / (1.0 + jnp.exp(-x))


def cost(flops, nbytes):
    return pl.CostEstimate(flops=int(flops), bytes_accessed=int(nbytes), transcendentals=0)


def terms(x, count):
    found = []
    for _ in range(count):
        found.append(x.astype(BF16))
        x = x - found[-1].astype(F32)
    return found


def whole(array):
    return pl.BlockSpec(array.shape, lambda *_: (0,) * array.ndim)


def places():
    tp, ep = lax.axis_index("tp"), lax.axis_index("ep")
    bits = jnp.arange(8)
    return jnp.where(bits < 4, tp ^ bits, jnp.where(bits == 4, ep % 2, ep // 2)).astype(jnp.int32)


def swap_tp(part, bit):
    return lax.ppermute(part, "tp", [(i, i ^ bit) for i in range(lax.axis_size("tp"))])


def swap_pair(part):
    return lax.ppermute(part, "ep", [(i, i ^ 1) for i in range(lax.axis_size("ep"))])


def shift_pairs(part, step, around):
    pairs = lax.axis_size("ep") // 2
    moves = []
    for pair in range(pairs):
        if around or 0 <= pair + step < pairs:
            moves += [(2 * pair + i, 2 * ((pair + step) % pairs) + i) for i in range(2)]
    return lax.ppermute(part, "ep", moves)


def gather_halves(x):
    half = x.shape[0] // 2
    near = swap_tp(x, 1)
    far = swap_tp(x, 2)
    low = swap_tp(far[:half], 1)
    high = swap_tp(near[half:], 2)
    return x, near, far, low, high


def gather_whole(x, last):
    near = swap_tp(x, 1)
    far = swap_tp(x, 2)
    source = {1: far, 2: near, 3: x}[last]
    return x, near, far, swap_tp(source, last)


def level_sums(size):
    t = np.arange(size)[:, None]
    u = np.arange(size)[None, :]
    mats = [u <= t]
    for h in (1, 2, 4):
        border = t // (2 * h) * (2 * h) + h - 1
        mats.append(np.where(t > border, (u > border) & (u <= t), (u > t) & (u <= border)))
    both = np.concatenate(mats, axis=0).astype(np.float32)
    return np.concatenate([both, both], axis=1)


def gates(preact, floor_logits, surge, head, width):
    row = lax.broadcasted_iota(jnp.int32, surge.shape, 0)
    mine = jnp.sum(jnp.where(row == head, surge, 0.0), axis=0, keepdims=True)
    stack = jnp.concatenate(terms(mine, 3) + [jnp.zeros((TAIL - 3, mine.shape[1]), BF16)], axis=0)
    column = dot_tn(stack, jnp.ones((TAIL, width), BF16))
    key = sigmoid(-floor_logits) * sigmoid(-preact.astype(F32))
    return key, jnp.log1p(-key) + column


def put_state(ref, at, state, decay):
    high, mid, low = terms(decay, 3)
    rows = state.shape[0]
    ref[at, :rows] = state.astype(BF16)
    ref[at, rows:] = jnp.concatenate([high, mid, low, jnp.zeros((TAIL - 3, state.shape[1]), BF16)], axis=0)


def get_state(packed):
    rows = packed.shape[0] - TAIL
    decay = packed[rows : rows + 3].astype(F32)
    return packed[:rows].astype(F32), decay[0:1] + decay[1:2] + decay[2:3]


def state_body(f_ref, v_ref, floor_ref, surge_ref, pre_ref, out_ref):
    key, g = gates(f_ref[...], floor_ref[...], surge_ref[...], pl.program_id(0), f_ref.shape[1])
    rows = g.shape[0]
    size = pre_ref.shape[0]
    prefix = []
    base = jnp.zeros((1, g.shape[1]), F32)
    for j in range(rows // size):
        part = dot_nn(pre_ref[...], jnp.concatenate(terms(g[j * size : (j + 1) * size], 2), axis=0)) + base
        base = part[size - 1 : size]
        prefix.append(part)
    prefix = jnp.concatenate(prefix, axis=0)
    weighted = (key * jnp.exp(base - prefix)).astype(BF16)
    put_state(out_ref, 0, dot_tn(v_ref[...], weighted), base)


def state_call(f, v, floor, surge):
    heads, rows = surge.shape
    width = f.shape[1] // heads
    vdim = v.shape[1] // heads
    size = min(CHUNK, rows)
    pre = jnp.asarray(level_sums(size)[:size], BF16)
    return pl.pallas_call(
        state_body,
        grid=(heads,),
        in_specs=[
            pl.BlockSpec((rows, width), lambda h: (0, h)),
            pl.BlockSpec((rows, vdim), lambda h: (0, h)),
            pl.BlockSpec((1, width), lambda h: (0, h)),
            whole(surge),
            whole(pre),
        ],
        out_specs=pl.BlockSpec((1, vdim + TAIL, width), lambda h: (h, 0, 0)),
        out_shape=jax.ShapeDtypeStruct((heads, vdim + TAIL, width), BF16),
        cost_estimate=cost(3e9, 2e6),
        name="state_end",
    )(f, v, floor, surge, pre)


def pair_body(at_ref, own_ref, other_ref, out_ref):
    second = at_ref[4] == 1
    for h in range(out_ref.shape[0]):
        own, own_decay = get_state(own_ref[h])
        other, other_decay = get_state(other_ref[h])
        later = jnp.where(second, own_decay, other_decay)
        first = jnp.where(second, other, own)
        last = jnp.where(second, own, other)
        put_state(out_ref, h, first * jnp.exp(later) + last, own_decay + other_decay)


def pair_call(at, own, other):
    heads, rows, width = own.shape
    half = pl.BlockSpec((heads // 2, rows, width), lambda i, at: (at[4], 0, 0))
    return pl.pallas_call(
        pair_body,
        grid_spec=pltpu.PrefetchScalarGridSpec(
            num_scalar_prefetch=1,
            grid=(1,),
            in_specs=[half, half],
            out_specs=pl.BlockSpec((heads // 2, rows, width), lambda i, at: (0, 0, 0)),
        ),
        out_shape=jax.ShapeDtypeStruct((heads // 2, rows, width), BF16),
        cost_estimate=cost(5e8, 1e6),
        name="pair_state",
    )(at, own, other)


def entering_body(*refs):
    *parts, out_ref = refs
    for h in range(out_ref.shape[0]):
        state = jnp.zeros(out_ref.shape[1:], F32)
        for part in reversed(parts):
            own, decay = get_state(part[h])
            state = state * jnp.exp(decay) + own
        out_ref[h] = state.astype(BF16)


def entering_call(parts):
    heads, rows, width = parts[0].shape
    return pl.pallas_call(
        entering_body,
        out_shape=jax.ShapeDtypeStruct((heads, rows - TAIL, width), BF16),
        cost_estimate=cost(5e8, 1e6),
        name="entering_state",
    )(*parts)


def recur_body(
    at_ref, q_ref, f_ref, v_ref, o_ref, floor_ref, surge_ref, gain_ref, mats_ref, mine_ref, theirs_ref, other_ref, out_ref
):
    head = pl.program_id(0)
    key, g = gates(f_ref[...], floor_ref[...], surge_ref[...], head, f_ref.shape[1])
    rows, width = g.shape
    size = mats_ref.shape[1] // 2
    here = at_ref[4] == head // (pl.num_programs(0) // 2)
    state = jnp.where(here, mine_ref[0], theirs_ref[0]).astype(F32)
    before, decay = get_state(other_ref[0])
    state = jnp.where(at_ref[4] == 1, state * jnp.exp(decay) + before, state)
    t = lax.broadcasted_iota(jnp.int32, (size, size), 0)
    s = lax.broadcasted_iota(jnp.int32, (size, size), 1)
    apart = jnp.where(t > s, t ^ s, jnp.where(t == s, 0, -1))
    row = lax.broadcasted_iota(jnp.int32, (size, width), 0)
    for j in range(rows // size):
        at = slice(j * size, (j + 1) * size)
        x = q_ref[at].astype(F32)
        q = x * sigmoid(x)
        k = key[at]
        v = v_ref[at]
        sums = dot_nn(mats_ref[...], jnp.concatenate(terms(g[at], 2), axis=0))
        prefix = sums[:size]
        total = prefix[size - 1 : size]
        scores = dot_nt(q.astype(BF16), k.astype(BF16))
        h = 1
        level = 1
        while h < size:
            if h < 8:
                z = jnp.where(row & h != 0, q, k) * jnp.exp(sums[level * size : (level + 1) * size])
            else:
                parts = []
                for low in range(0, size, 2 * h):
                    mid = low + h
                    border = prefix[mid - 1 : mid]
                    parts.append(k[low:mid] * jnp.exp(border - prefix[low:mid]))
                    parts.append(q[mid : mid + h] * jnp.exp(prefix[mid : mid + h] - border))
                z = jnp.concatenate(parts, axis=0)
            z = z.astype(BF16)
            scores = jnp.where(apart >= h, dot_nt(z, z), scores)
            h *= 2
            level += 1
        scores = jnp.where(apart >= 0, scores, 0.0).astype(BF16)
        out = dot_nn(scores, v) + dot_nt((q * jnp.exp(prefix)).astype(BF16), state.astype(BF16))
        state = state * jnp.exp(total) + dot_tn(v, (k * jnp.exp(total - prefix)).astype(BF16))
        gate = o_ref[at].astype(F32)
        scale = lax.rsqrt(jnp.mean(out * out, axis=1, keepdims=True) + NORM_EPS)
        out_ref[at] = (out * scale * gain_ref[...] * (gate * sigmoid(gate))).astype(BF16)


def recur_call(at, q, f, v, o, floor, surge, gain, mine, theirs, other):
    heads, rows = surge.shape
    width = f.shape[1] // heads
    vdim = v.shape[1] // heads
    half = heads // 2
    mats = jnp.asarray(level_sums(min(CHUNK, rows)), BF16)

    def tall(n):
        return pl.BlockSpec((rows, n), lambda h, at: (0, h))

    return pl.pallas_call(
        recur_body,
        grid_spec=pltpu.PrefetchScalarGridSpec(
            num_scalar_prefetch=1,
            grid=(heads,),
            in_specs=[
                tall(width),
                tall(width),
                tall(vdim),
                tall(vdim),
                pl.BlockSpec((1, width), lambda h, at: (0, h)),
                whole(surge),
                whole(gain),
                whole(mats),
                pl.BlockSpec((1, vdim, width), lambda h, at: (h % half, 0, 0)),
                pl.BlockSpec((1, vdim, width), lambda h, at: (h % half, 0, 0)),
                pl.BlockSpec((1, vdim + TAIL, width), lambda h, at: (h, 0, 0)),
            ],
            out_specs=tall(vdim),
        ),
        out_shape=jax.ShapeDtypeStruct((rows, heads * vdim), BF16),
        cost_estimate=cost(6e9, 4e6),
        name="recurrence",
    )(at, q, f, v, o, floor, surge, gain, mats, mine, theirs, other)


IN_HBM = pl.BlockSpec(memory_space=pltpu.HBM)
IN_PLACE = pl.BlockSpec(memory_space=pl.ANY)


def fetch(source, target, sem):
    copy = pltpu.make_async_copy(source, target, sem)
    copy.start()
    return copy


def project_call(at, pieces, weight):
    rows, inner = pieces[0].shape
    columns = weight.shape[1]
    half = rows // 2

    def body(at_ref, w_hbm, own, near, far, low, high, out_ref, x_ref, fourth_ref, w_ref, x_sem, w_sem):
        weights = []
        copies = []
        for p in range(4):
            begin = pl.ds(pl.multiple_of(at_ref[p] * inner, inner), inner)
            weights.append(fetch(w_hbm.at[begin, :], w_ref.at[p], w_sem.at[p]))
            if p < 3:
                copies.append([fetch((own, near, far)[p], x_ref.at[p], x_sem.at[p])])
            else:
                copies.append([fetch(ref, fourth_ref.at[i], x_sem.at[3 + i]) for i, ref in enumerate((low, high))])
        accs = [jnp.zeros((half, columns), F32)] * 2
        for p in range(4):
            weights[p].wait()
            for copy in copies[p]:
                copy.wait()
            for side in range(2):
                lhs = x_ref[p, side * half : (side + 1) * half] if p < 3 else fourth_ref[side]
                accs[side] += dot_nn(lhs, w_ref[p])
        for side in range(2):
            out_ref[side * half : (side + 1) * half] = accs[side].astype(BF16)

    return pl.pallas_call(
        body,
        grid_spec=pltpu.PrefetchScalarGridSpec(
            num_scalar_prefetch=1,
            grid=(1,),
            in_specs=[IN_HBM] + [IN_PLACE] * 5,
            out_specs=pl.BlockSpec((rows, columns), lambda i, at: (0, 0)),
            scratch_shapes=[
                pltpu.VMEM((3, rows, inner), BF16),
                pltpu.VMEM((2, half, inner), BF16),
                pltpu.VMEM((4, inner, columns), BF16),
                pltpu.SemaphoreType.DMA((5,)),
                pltpu.SemaphoreType.DMA((4,)),
            ],
        ),
        out_shape=jax.ShapeDtypeStruct((rows, columns), BF16),
        cost_estimate=cost(2 * rows * weight.shape[0] * columns, 4e6),
        name="mix_project",
    )(at, weight, *pieces)


def room_of(group, pair, room):
    rows = group.shape[1]
    ahead = group - pair
    ahead = jnp.where(ahead < 0, ahead + GROUPS, ahead)
    kind = lax.broadcasted_iota(jnp.int32, (8, rows), 0)
    named = jnp.where(kind == ahead, 1.0, 0.0)
    u = lax.broadcasted_iota(jnp.int32, (rows, rows), 0)
    r = lax.broadcasted_iota(jnp.int32, (rows, rows), 1)
    earlier = jnp.where(u < r, 1.0, 0.0).astype(BF16)
    rank = jnp.sum(dot_nn(named.astype(BF16), earlier) * named, axis=0, keepdims=True)
    slot = ahead * room + rank.astype(jnp.int32)
    at = lax.broadcasted_iota(jnp.int32, (GROUPS * room, rows), 0)
    return jnp.where(at == slot, 1.0, 0.0).astype(BF16)


def route_body(at_ref, x_ref, gain_ref, group_ref, index_ref, weight_ref, *refs):
    *outs, normed_ref = refs
    x = x_ref[...].astype(F32)
    scale = lax.rsqrt(jnp.mean(x * x, axis=1, keepdims=True) + NORM_EPS)
    normed = (x * scale * gain_ref[...]).astype(BF16)
    columns = normed_ref.shape[2]
    for i in range(normed_ref.shape[0]):
        normed_ref[i] = normed[:, i * columns : (i + 1) * columns]
    room = outs[0].shape[0]
    chosen = room_of(group_ref[...], at_ref[5], room)
    rows = chosen.shape[1]
    index = (index_ref[...] + 1).astype(F32).astype(BF16)
    weight = terms(weight_ref[...], 3)
    notes = jnp.concatenate([index] + weight + [jnp.zeros((outs[0].shape[1] - columns - 8, rows), BF16)], axis=0)
    body = dot_nn(chosen, normed_ref[at_ref[0]]).astype(BF16)
    notes = dot_nt(chosen, notes).astype(BF16)
    for i, out in enumerate(outs):
        out[:, :columns] = body[i * room : (i + 1) * room]
        out[:, columns:] = notes[i * room : (i + 1) * room]


def route_call(at, x, gain, group, index, weight, room):
    rows, width = x.shape
    tp = lax.axis_size("tp")
    columns = width // tp
    block = (room, columns + 128)
    return pl.pallas_call(
        route_body,
        grid_spec=pltpu.PrefetchScalarGridSpec(
            num_scalar_prefetch=1,
            grid=(1,),
            in_specs=[whole(x), whole(gain), whole(group), whole(index), whole(weight)],
            out_specs=[pl.BlockSpec(block, lambda i, at: (0, 0))] * GROUPS,
            scratch_shapes=[pltpu.VMEM((tp, rows, columns), BF16)],
        ),
        out_shape=[jax.ShapeDtypeStruct(block, BF16)] * GROUPS,
        cost_estimate=cost(1e9, 2e6),
        name="route_rows",
    )(at, x, gain, group, index, weight)


def stack_body(*refs):
    *parts, rows_ref, pack_ref = refs
    room = parts[0].shape[0]
    columns = rows_ref.shape[1]
    for i, part in enumerate(parts):
        rows_ref[i * room : (i + 1) * room] = part[:, :columns]
        pack_ref[i * room : (i + 1) * room] = part[...]


def stack_call(parts):
    room, width = parts[0].shape
    rows = room * len(parts)
    return pl.pallas_call(
        stack_body,
        out_shape=[jax.ShapeDtypeStruct((rows, width - 128), BF16), jax.ShapeDtypeStruct((rows, width), BF16)],
        cost_estimate=cost(2e8, 1e6),
        name="stack_rows",
    )(*parts)


def choices_of(notes, core, local, begin, count):
    rows = notes.shape[0]
    lane = lax.broadcasted_iota(jnp.int32, notes.shape, 1)
    choice = notes.astype(jnp.int32) - 1 - core * local - begin
    first = (lane == choice[:, 0:1]) & (lane < count)
    second = (lane == choice[:, 1:2]) & (lane < count)
    named = jnp.where(first | second, 1.0, 0.0)
    t = lax.broadcasted_iota(jnp.int32, (rows, rows), 0)
    u = lax.broadcasted_iota(jnp.int32, (rows, rows), 1)
    earlier = jnp.where(u < t, 1.0, 0.0).astype(BF16)
    rank = (dot_nn(earlier, named.astype(BF16)) * named).astype(BF16)
    return first, second, named.astype(BF16), rank


def slot_numbers(count, each):
    number = np.arange(count * each)
    pick = jnp.asarray(number[:, None] // each == np.arange(128)[None, :], BF16)
    down = jnp.asarray(np.broadcast_to((number % each)[:, None], (count * each, 128)), F32)
    return pick, down, jnp.asarray((number % each)[None, :], F32)


def mixes_call(at, packs, local, each):
    room, width = packs[0].shape
    rows = room * len(packs)
    slots = local * each
    pick, _, across = slot_numbers(local, each)

    def body(at_ref, pick_ref, across_ref, *refs):
        outs = refs[len(packs) :]
        notes = jnp.concatenate([ref[...] for ref in refs[: len(packs)]], axis=0).astype(F32)
        first, second, named, rank = choices_of(notes, at_ref[4], local, 0, local)
        pick = pick_ref[...]
        given = (dot_nt(named, pick) > 0.5) & (dot_nt(rank, pick) == across_ref[...])
        for i, ref in enumerate(outs):
            begin = 2 + 2 * i
            weight = jnp.where(first, notes[:, begin : begin + 1], 0.0) + jnp.where(
                second, notes[:, begin + 1 : begin + 2], 0.0
            )
            ref[...] = jnp.where(given, dot_nt(weight.astype(BF16), pick), 0.0).astype(BF16)

    last = width // 128 - 1
    return pl.pallas_call(
        body,
        grid_spec=pltpu.PrefetchScalarGridSpec(
            num_scalar_prefetch=1,
            grid=(1,),
            in_specs=[whole(pick), whole(across)]
            + [pl.BlockSpec((room, 128), lambda i, at: (0, last))] * len(packs),
            out_specs=[pl.BlockSpec((rows, slots), lambda i, at: (0, 0))] * 2,
        ),
        out_shape=[jax.ShapeDtypeStruct((rows, slots), BF16)] * 2,
        cost_estimate=cost(1e9, 2e6),
        name="expert_mixes",
    )(at, pick, across, *packs)


def hidden_call(at, own, other, gate_w, up_w, each):
    local, width, units = gate_w.shape
    pieces = [*own, *other]
    ways = len(own)
    columns = own[1].shape[1]
    slots = local * each
    half = local // 2
    pick, down, _ = slot_numbers(local, each)

    def body(at_ref, pick_ref, down_ref, *refs):
        sources = refs[: len(pieces)]
        gate_ref, up_ref, first_ref, second_ref, x_ref = refs[len(pieces) :]
        e = pl.program_id(0)

        @pl.when(e == 0)
        def _():
            notes = jnp.concatenate([sources[0][:, columns:], sources[ways][:, columns:]], axis=0).astype(F32)
            _, _, named, rank = choices_of(notes, at_ref[4], local, 0, local)
            pick = pick_ref[...]
            taken = (dot_nt(pick, named) > 0.5) & (dot_nt(pick, rank) == down_ref[:, 0:1])
            take = jnp.where(taken, 1.0, 0.0).astype(BF16)
            for p in range(ways):
                part = jnp.concatenate([sources[p][:, :columns], sources[ways + p][:, :columns]], axis=0)
                lanes = pl.ds(pl.multiple_of(at_ref[p] * columns, columns), columns)
                x_ref[:, lanes] = dot_nn(take, part).astype(BF16)

        x = x_ref[pl.ds(pl.multiple_of(e * each, each), each), :]
        gate = dot_nn(x, gate_ref[0])
        up = dot_nn(x, up_ref[0])
        value = (gate * sigmoid(gate) * up).astype(BF16)

        @pl.when(e < half)
        def _():
            first_ref[...] = value

        @pl.when(e >= half)
        def _():
            second_ref[...] = value

    return pl.pallas_call(
        body,
        grid_spec=pltpu.PrefetchScalarGridSpec(
            num_scalar_prefetch=1,
            grid=(local,),
            in_specs=[whole(pick), whole(down)]
            + [whole(part) for part in pieces]
            + [pl.BlockSpec((1, width, units), lambda e, at: (e, 0, 0))] * 2,
            out_specs=[
                pl.BlockSpec((each, units), lambda e, at: (jnp.minimum(e, half - 1), 0)),
                pl.BlockSpec((each, units), lambda e, at: (jnp.maximum(e - half, 0), 0)),
            ],
            scratch_shapes=[pltpu.VMEM((slots, width), BF16)],
        ),
        out_shape=[jax.ShapeDtypeStruct((slots // 2, units), BF16)] * 2,
        cost_estimate=cost(1e10, 4 * local * width * units),
        name="expert_hidden",
    )(at, pick, down, *pieces, gate_w, up_w)


def result_call(at, pieces, down_w, begin, before=None, mixes=None):
    _, inner, columns = down_w.shape
    slots, units = pieces[0].shape
    count = 2
    each = slots // count
    extra = [] if before is None else [before, *mixes]

    def body(at_ref, *refs):
        down_ref = refs[4]
        given = refs[5 : 5 + len(extra)]
        outs = refs[5 + len(extra) : -4]
        x_ref, w_ref, x_sem, w_sem = refs[-4:]
        copies = [fetch(ref, x_ref.at[i], x_sem.at[i]) for i, ref in enumerate(refs[:4])]

        def weight(i):
            rows = pl.ds(pl.multiple_of(at_ref[i % 4] * units, units), units)
            return fetch(down_ref.at[begin + i // 4, rows, :], w_ref.at[i], w_sem.at[i])

        ahead = 5
        weights = [weight(i) for i in range(ahead)]
        for copy in copies:
            copy.wait()
        results = []
        for e in range(count):
            span = slice(e * each, (e + 1) * each)
            acc = jnp.zeros((each, columns), F32)
            for p in range(4):
                weights[4 * e + p].wait()
                if 4 * e + p + ahead < 4 * count:
                    weights.append(weight(4 * e + p + ahead))
                acc += dot_nn(x_ref[p, span], w_ref[4 * e + p])
            results.append(acc.astype(BF16))
        if not extra:
            outs[0][...] = jnp.concatenate(results, axis=0)
        else:
            result = jnp.concatenate([given[0][...]] + results, axis=0)
            total = dot_nn(given[1][...], result) + dot_nn(given[2][...], result)
            half = total.shape[0] // 2
            outs[0][...] = total[:half]
            outs[1][...] = total[half:].astype(BF16)

    if not extra:
        shapes = [jax.ShapeDtypeStruct((slots, columns), BF16)]
    else:
        half = mixes[0].shape[0] // 2
        shapes = [jax.ShapeDtypeStruct((half, columns), F32), jax.ShapeDtypeStruct((half, columns), BF16)]
    return pl.pallas_call(
        body,
        grid_spec=pltpu.PrefetchScalarGridSpec(
            num_scalar_prefetch=1,
            grid=(1,),
            in_specs=[IN_PLACE] * 4 + [IN_HBM] + [whole(array) for array in extra],
            out_specs=[pl.BlockSpec(shape.shape, lambda i, at: (0, 0)) for shape in shapes],
            scratch_shapes=[
                pltpu.VMEM((4, slots, units), BF16),
                pltpu.VMEM((count * 4, units, columns), BF16),
                pltpu.SemaphoreType.DMA((4,)),
                pltpu.SemaphoreType.DMA((count * 4,)),
            ],
        ),
        out_shape=shapes,
        cost_estimate=cost(2.5e9, 2 * count * inner * columns),
        name="expert_result",
    )(at, *pieces, down_w, *extra)


def add_body(kept_ref, came_ref, *outs):
    total = (kept_ref[...] + came_ref[...].astype(F32)).astype(BF16)
    room = outs[0].shape[0]
    for i, out in enumerate(outs):
        out[...] = total[i * room : (i + 1) * room]


def add_call(kept, came, room):
    block = (room, kept.shape[1])
    return pl.pallas_call(
        add_body,
        out_shape=[jax.ShapeDtypeStruct(block, BF16)] * (kept.shape[0] // room),
        cost_estimate=cost(2e8, 1e6),
        name="add_shares",
    )(kept, came)


def return_body(at_ref, group_ref, *refs):
    *parts, out_ref = refs
    chosen = room_of(group_ref[...], at_ref[5], parts[0].shape[0])
    back = jnp.concatenate([part[...] for part in parts], axis=0)
    out_ref[...] = dot_tn(chosen, back).astype(BF16)


def return_call(at, group, parts):
    rows = group.shape[1]
    columns = parts[0].shape[1]
    return pl.pallas_call(
        return_body,
        grid_spec=pltpu.PrefetchScalarGridSpec(
            num_scalar_prefetch=1,
            grid=(1,),
            in_specs=[whole(group)] + [whole(part) for part in parts],
            out_specs=pl.BlockSpec((rows, columns), lambda i, at: (0, 0)),
        ),
        out_shape=jax.ShapeDtypeStruct((rows, columns), BF16),
        cost_estimate=cost(5e8, 1e6),
        name="return_rows",
    )(at, group, *parts)


def paired(
    recurrence_queries,
    forget_preact,
    recurrence_values,
    output_gate_preact,
    forget_floor_logits,
    surge_log_decay,
    head_norm_gain,
    recurrence_out_weight,
    second_micro_rows,
    expert_norm_gain,
    row_group_index,
    group_expert_index,
    chosen_expert_weight,
    expert_gate_weight,
    expert_up_weight,
    expert_down_weight,
):
    pairs = lax.axis_size("ep") // 2
    local_experts = expert_gate_weight.shape[0]
    room = 2 * local_experts * CAP // 2
    at = places()
    group = row_group_index.reshape(1, -1)
    floor = forget_floor_logits.reshape(1, -1)
    surge = surge_log_decay.T

    blocks = route_call(
        at,
        second_micro_rows,
        expert_norm_gain.reshape(1, -1),
        group,
        group_expert_index.T,
        chosen_expert_weight.T,
        room,
    )
    *blocks, early_floor = lax.optimization_barrier((*blocks, floor))
    ending = state_call(forget_preact, recurrence_values, early_floor, surge)
    blocks = [blocks[0]] + [shift_pairs(blocks[i], i, True) for i in range(1, pairs)]
    rows, pack = stack_call(blocks)
    _, *rest = gather_whole(rows, 3)
    own = [pack, *rest]
    other = [swap_pair(part) for part in own]
    other_ending = swap_pair(ending)
    ended = pair_call(at, ending, other_ending)
    states = [shift_pairs(ended, i, False) for i in range(1, pairs)]
    each = 2 * pairs * CAP
    half = local_experts // 2
    hidden = hidden_call(at, own, other, expert_gate_weight, expert_up_weight, each)
    *states, late_floor, _ = lax.optimization_barrier((*states, floor, hidden[0]))
    mine = entering_call(states)
    theirs = swap_pair(mine)
    units = [gather_whole(part, 2 - i) for i, part in enumerate(hidden)]

    gated = recur_call(
        at,
        recurrence_queries,
        forget_preact,
        recurrence_values,
        output_gate_preact,
        late_floor,
        surge,
        head_norm_gain.reshape(1, -1),
        mine,
        theirs,
        other_ending,
    )
    heads = gather_halves(gated)
    mixes = mixes_call(at, (own[0], other[0]), local_experts, each)
    mixed = project_call(at, heads, recurrence_out_weight)
    (early,) = result_call(at, units[0], expert_down_weight, 0)
    kept, sent = result_call(at, units[1], expert_down_weight, half, early, mixes)
    shares = add_call(kept, swap_pair(sent), room)
    back = [shares[0]] + [shift_pairs(shares[i], -i, True) for i in range(1, pairs)]
    return (mixed, return_call(at, group, back))


def in_layer(*args):
    return paired(*args)


def solution(mesh):
    pairs = mesh.shape["ep"] == 2 * GROUPS and mesh.shape["tp"] == 4
    return jax.shard_map(
        in_layer if pairs else plain,
        mesh=mesh,
        in_specs=(
            P("ep", "tp"),
            P("ep", "tp"),
            P("ep", "tp"),
            P("ep", "tp"),
            P("tp"),
            P("ep", "tp"),
            P(),
            P(None, "tp"),
            P("ep", None),
            P(),
            P("ep"),
            P("ep", None),
            P("ep", None),
            P("ep", None, "tp"),
            P("ep", None, "tp"),
            P("ep", None, "tp"),
        ),
        out_specs=(P("ep", "tp"), P("ep", "tp")),
        check_vma=False,
    )
```
